32 devices in a mesh: kv: 16 (over z, y, x), tp: 2 (over core).
Axes of the slice: x: 2, y: 2, z: 4, core: 2. Of those that a mesh axis runs over, the one named last changes fastest.
Arguments:
- queries: bfloat16 [2048, 1024], P('kv', 'tp'), may hold values from -4 to 4
- keys: bfloat16 [2048, 1024], P('kv', 'tp'), may hold values from -4 to 4
- values: bfloat16 [2048, 1024], P('kv', 'tp'), may hold values from -4 to 4
- cotangent: bfloat16 [2048, 1024], P('kv', 'tp'), may hold values from -4 to 4
- log_sum: float32 [16, 2048], P('tp', 'kv'), may hold values from 4.5 to 7.5
- chosen: int32 [16, 64, 12], P('tp'), may hold values from 0 to 63, as said below
- normed_input: bfloat16 [2048, 2048], P('kv', 'tp'), may hold values from -0.125 to 0.125
Outputs:
- grad_queries: bfloat16 [2048, 1024], P('kv', 'tp')
- grad_keys: bfloat16 [2048, 1024], P('kv', 'tp')
- grad_values: bfloat16 [2048, 1024], P('kv', 'tp')
- grad_weight: float32 [2048, 1024], P('kv', 'tp')
The draws below stay inside these ranges and needn't reach their ends.
Inputs may be any that keep to these rules, and one draw needn't show every extreme that they name: `chosen`: for each head, the distinct blocks below their own query block that the query blocks of one device's 128 positions choose include at most 1 block of any one device's span of 128 positions, and exactly 1 for some pairs of devices. Within one list the entries below the query block's own index are distinct.
All inputs are finite; a program needn't handle non-finite values.
Results may differ from the reference program's by a relative error of at most 0.0085.
Values may be sent and summed in bfloat16 or wider, within the bound.
A program may use at most 64 MiB of HBM per device.

```python
import jax
import jax.numpy as jnp
from jax import lax

D = 2048
HEADS = 16
HD = 64
BLK = 32
SEL = 12
MOST = 1
TOK_DEV = 128
TOKENS = 2048
WIDTH = 1024
N_KV = 16


def draw_chosen(key, part):
    devices = N_KV
    blocks_dev = TOK_DEV // BLK
    splits = jax.random.split(jax.random.fold_in(key, 17), 4)
    first_pick = jax.random.randint(splits[0], (HEADS, devices, devices), 0, blocks_dev)
    step_pick = jax.random.randint(splits[1], (HEADS, devices, devices), 1, blocks_dev)
    owner_ids = jnp.arange(devices, dtype=jnp.int32)
    cand_list = []
    for slot_index in range(MOST):
        local_pick = (first_pick + slot_index * step_pick) % blocks_dev
        cand_list.append(owner_ids[None, None, :] * blocks_dev + local_pick)
    candidates = jnp.stack(cand_list, axis=-1)
    popular = jax.random.randint(splits[2], (HEADS, 1, devices, 1), 0, 8)
    popular = popular * popular
    query_dev = owner_ids[None, :, None, None]
    owner_dev = owner_ids[None, None, :, None]
    boosted = jnp.where((owner_dev == query_dev - 1) | (owner_dev == query_dev - devices // 2), 2, 0)
    base_score = boosted * 64 + popular
    jitter = jax.random.randint(splits[3], (HEADS, devices, blocks_dev, devices, MOST), 0, 4096)
    query_ids = owner_ids[:, None] * blocks_dev + jnp.arange(blocks_dev, dtype=jnp.int32)[None, :]
    cand_rows = candidates[:, :, None, :, :]
    usable = cand_rows < query_ids[None, :, :, None, None]
    tie_break = jnp.arange(MOST * devices, dtype=jnp.int32).reshape(devices, MOST)
    scored = (base_score[:, :, None, :, :] * 4096 + jitter) * 256 + tie_break
    scored = jnp.where(usable, scored, -1).reshape(HEADS, devices, blocks_dev, MOST * devices)
    top_values, top_index = lax.top_k(scored, SEL)
    flat_cands = jnp.broadcast_to(cand_rows, (HEADS, devices, blocks_dev, devices, MOST)).reshape(HEADS, devices, blocks_dev, MOST * devices)
    picked = jnp.take_along_axis(flat_cands, top_index, axis=-1)
    picked = jnp.where(top_values >= 0, picked, query_ids[None, :, :, None])
    return picked.reshape(HEADS, devices * blocks_dev, SEL).astype(jnp.int32)


def block_levels(stream_key, shape, cuts, low, largest):
    level, own = 1.0, jax.random.fold_in(stream_key, 6)
    for dim, blocks in cuts:
        draws = jnp.exp(jax.random.uniform(jax.random.fold_in(own, dim), (blocks,), jnp.float32, low / len(cuts), largest / len(cuts)))
        level = level * jnp.repeat(draws, shape[dim] // blocks).reshape([-1 if axis == dim else 1 for axis in range(len(shape))])
    return level


def noise(own_key, shape, scale, most, pieces=(), kind=jnp.bfloat16):
    gain = block_levels(own_key, shape, pieces, -0.22, 0.18) if pieces else 1.0
    array = jax.random.normal(own_key, shape, jnp.float32) * scale * gain
    return jnp.minimum(jnp.maximum(array, -most), most).astype(kind)


def setup_inputs(seed: int = 0) -> dict:
    key_list = jax.random.split(jax.random.key(seed), 8)
    queries = noise(key_list[0], (TOKENS, WIDTH), 1.0, 4.0, ((0, 16), (1, 2)))
    keys = noise(key_list[1], (TOKENS, WIDTH), 1.0, 4.0, ((0, 16), (1, 2)))
    values = noise(key_list[2], (TOKENS, WIDTH), 1.0, 4.0, ((0, 16), (1, 2)))
    cotangent = noise(key_list[3], (TOKENS, WIDTH), 1.0, 4.0, ((0, 16), (1, 2)))
    log_sum = jnp.clip(4.5 + 3.0 * jax.random.uniform(key_list[4], (HEADS, TOKENS), jnp.float32) ** block_levels(key_list[4], (HEADS, TOKENS), ((0, 2), (1, 16)), -0.2, 0.2), 4.5, 7.5)
    chosen = draw_chosen(jax.random.fold_in(key_list[7], 71), 0)
    normed_input = noise(key_list[6], (TOKENS, D), TOKENS ** -0.5, 0.125, ((0, 16), (1, 2)))
    return dict(queries=queries, keys=keys, values=values, cotangent=cotangent, log_sum=log_sum, chosen=chosen, normed_input=normed_input)


MASKED = -1e30


def reference(queries, keys, values, cotangent, log_sum, chosen, normed_input):
    token_count = queries.shape[0]
    block_total = token_count // BLK
    score_scale = HD ** -0.5
    block_ids = jnp.arange(block_total, dtype=jnp.int32)
    causal = jnp.arange(BLK)[:, None] >= jnp.arange(BLK)[None, :]

    def per_head(head_index):
        def columns(row_block):
            picked_cols = lax.dynamic_slice_in_dim(row_block, head_index * HD, HD, 1)
            return picked_cols.reshape(block_total, BLK, HD).astype(jnp.float32)

        q_blocks = columns(queries)
        k_blocks = columns(keys)
        v_blocks = columns(values)
        g_blocks = columns(cotangent)
        log_rows = lax.dynamic_index_in_dim(log_sum, head_index, 0, keepdims=False).reshape(block_total, BLK)[..., None]
        picked = lax.dynamic_index_in_dim(chosen, head_index, 0, keepdims=False).astype(jnp.int32)
        usable = picked < block_ids[:, None]
        safe_ids = jnp.where(usable, picked, 0).astype(jnp.int32)
        keys_all = jnp.concatenate([k_blocks[safe_ids].reshape(block_total, SEL * BLK, HD), k_blocks], axis=1)
        values_all = jnp.concatenate([v_blocks[safe_ids].reshape(block_total, SEL * BLK, HD), v_blocks], axis=1)
        sel_mask = jnp.broadcast_to(jnp.repeat(usable, BLK, axis=1)[:, None, :], (block_total, BLK, SEL * BLK))
        allowed = jnp.concatenate([sel_mask, jnp.broadcast_to(causal, (block_total, BLK, BLK))], axis=2)
        scores = jnp.einsum('jqd,jkd->jqk', q_blocks, keys_all) * score_scale
        weights = jnp.exp(jnp.where(allowed, scores - log_rows, MASKED))
        value_dots = jnp.einsum('jqd,jkd->jqk', g_blocks, values_all)
        row_delta = jnp.sum(weights * value_dots, axis=-1, keepdims=True)
        score_grad = lax.optimization_barrier((weights * (value_dots - row_delta)).astype(jnp.bfloat16)).astype(jnp.float32)
        weights_low = lax.optimization_barrier(weights.astype(jnp.bfloat16)).astype(jnp.float32)
        query_grad = jnp.einsum('jqk,jkd->jqd', score_grad, keys_all) * score_scale
        key_grad = jnp.einsum('jqk,jqd->jkd', score_grad, q_blocks) * score_scale
        value_grad = jnp.einsum('jqk,jqd->jkd', weights_low, g_blocks)

        def settle(gradient):
            spread = gradient[:, :SEL * BLK].reshape(block_total * SEL, BLK, HD)
            summed = jax.ops.segment_sum(spread, safe_ids.reshape(-1), num_segments=block_total)
            return (summed + gradient[:, SEL * BLK:]).reshape(token_count, HD).astype(jnp.bfloat16)

        return query_grad.reshape(token_count, HD).astype(jnp.bfloat16), settle(key_grad), settle(value_grad)

    head_grads = lax.map(per_head, jnp.arange(HEADS, dtype=jnp.int32))

    def joined_rows(stacked):
        return stacked.transpose(1, 0, 2).reshape(token_count, HEADS * HD)

    grad_queries = joined_rows(head_grads[0])
    grad_keys = joined_rows(head_grads[1])
    grad_values = joined_rows(head_grads[2])
    grad_weight = jnp.dot(normed_input.T, grad_queries, preferred_element_type=jnp.float32)
    return grad_queries, grad_keys, grad_values, grad_weight
```

```python
import functools

import jax
import jax.numpy as jnp
from jax import lax
from jax.experimental import pallas as pl
from jax.experimental.pallas import tpu as pltpu
from jax.sharding import PartitionSpec as P

HD = 64
BLK = 32
MASKED = -1e30
MESH = pl.DeviceIdType.MESH
F32 = jnp.float32
BF16 = jnp.bfloat16


def dot(a, b, ca, cb):
    return lax.dot_general(a, b, (((ca,), (cb,)), ((), ())), preferred_element_type=F32)


def kernel(
    n, tp, g, q_ref, k_ref, v_ref, c_ref, bias_ref, hot_ref, x_ref,
    gq_ref, gk_ref, gv_ref, gw_ref,
    ks, vs, kt, vt, dvs, dks, dvr, dkr, wt, wo, gko, gvo, qs, cs, xs, xr, dqr, gs, gr,
    ssem, rsem, xssem, xrsem, gssem, grsem,
):
    r = n // g
    tok, cols = q_ref.shape
    bd = tok // BLK
    pairs = cols // (2 * HD)
    wide = 2 * HD
    scale = HD ** (-0.5)
    rt = r // tp
    w = x_ref.shape[1] // (rt * g)
    me, t = lax.axis_index("kv"), lax.axis_index("tp")
    z, j = me // g, lax.rem(me, g)

    def tile_copy(kind, src, dst, there, slot):
        return pltpu.make_async_remote_copy(
            src_ref=src, dst_ref=dst, send_sem=ssem.at[kind, there], recv_sem=rsem.at[kind, slot],
            device_id=(there, t), device_id_type=MESH)

    def picked(ref, d):
        out = None
        for b in range(bd):
            hot = jnp.broadcast_to(hot_ref[d, b : b + 1, :], (BLK, cols)).astype(BF16)
            term = ref[b * BLK : (b + 1) * BLK, :] * hot
            out = term if out is None else out + term
        return out

    def send_all(kind, ref, buf, landing):
        def step(i, carry):
            d = n - 1 - i
            buf[d] = picked(ref, d)
            tile_copy(kind, buf.at[d], landing.at[me], d, me).start()
            return carry
        lax.fori_loop(0, n - 1 - me, step, 0)

    def each_lower(fn):
        def step(o, carry):
            fn(o)
            return carry
        lax.fori_loop(0, me, step, 0)

    def each_upper(fn):
        def step(d, carry):
            fn(d)
            return carry
        lax.fori_loop(me + 1, n, step, 0)

    send_all(0, k_ref, ks, kt)
    send_all(1, v_ref, vs, vt)

    def clear(o, carry):
        kt[o] = jnp.zeros(kt.shape[1:], BF16)
        vt[o] = jnp.zeros(vt.shape[1:], BF16)
        return carry
    lax.fori_loop(me, n, clear, 0)

    for p in range(g):
        for zl in range(rt):
            at = (zl * g + p) * w
            xs[p, zl] = x_ref[:, at : at + w]

    def x_copy(p, t2):
        return pltpu.make_async_remote_copy(
            src_ref=xs.at[p], dst_ref=xr.at[j, pl.ds(t * rt, rt)],
            send_sem=xssem.at[p, t2], recv_sem=xrsem.at[j, t],
            device_id=(z * g + p, t2), device_id_type=MESH)

    def x_landed(p, t2):
        return pltpu.make_async_remote_copy(
            src_ref=xs.at[p], dst_ref=xr.at[p, pl.ds(t2 * rt, rt)],
            send_sem=xssem.at[p, t2], recv_sem=xrsem.at[p, t2],
            device_id=(z * g + p, t2), device_id_type=MESH)

    def each_x(fn):
        def step(i, carry):
            p, t2 = i // tp, lax.rem(i, tp)

            @pl.when((p != j) | (t2 != t))
            def _():
                fn(p, t2)
            return carry
        lax.fori_loop(0, g * tp, step, 0)

    each_x(lambda p, t2: x_copy(p, t2).start())
    xr[j, pl.ds(t * rt, rt)] = xs[j]

    low = lax.broadcasted_iota(jnp.int32, (tok, wide), 1) < HD
    for h in range(pairs):
        c = h * wide
        qp, cp = q_ref[:, c : c + wide], c_ref[:, c : c + wide]
        zero = jnp.zeros_like(qp)
        qs[h, :tok], qs[h, tok:] = jnp.where(low, qp, zero), jnp.where(low, zero, qp)
        cs[h, :tok], cs[h, tok:] = jnp.where(low, cp, zero), jnp.where(low, zero, cp)

    key_at = lax.broadcasted_iota(jnp.int32, (tok, 2 * tok), 0)
    query_at = lax.rem(lax.broadcasted_iota(jnp.int32, (tok, 2 * tok), 1), tok)
    causal = (key_at // BLK == query_at // BLK) & (key_at <= query_at)
    rows = n * BLK

    for h in range(pairs):
        c = h * wide
        so = dot(k_ref[:, c : c + wide], qs[h], 1, 1) * scale
        ob = jnp.broadcast_to(bias_ref[h, n : n + bd], (bd, BLK, 2 * tok)).reshape(tok, 2 * tok)
        ob = jnp.where(causal, bias_ref[h, n + bd], ob)
        weights = jnp.exp(so + ob)
        wo[h] = weights
        gvo[:, c : c + wide] = dot(weights.astype(BF16), cs[h], 1, 0)

    each_lower(lambda o: tile_copy(0, ks.at[o], kt.at[o], o, o).wait_recv())
    for h in range(pairs):
        c = h * wide
        kp = kt[:, :, c : c + wide].reshape(rows, wide)
        st = (dot(kp, qs[h], 1, 1) * scale).reshape(n, BLK, 2 * tok)
        weights = jnp.exp(st + bias_ref[h, :n]).reshape(rows, 2 * tok)
        wt[h] = weights
        dvs[:, :, c : c + wide] = dot(weights.astype(BF16), cs[h], 1, 0).astype(BF16).reshape(n, BLK, wide)
    each_lower(lambda o: tile_copy(2, dvs.at[o], dvr.at[me], o, me).start())

    each_lower(lambda o: tile_copy(1, vs.at[o], vt.at[o], o, o).wait_recv())
    for h in range(pairs):
        c = h * wide
        vp = vt[:, :, c : c + wide].reshape(rows, wide)
        kp = kt[:, :, c : c + wide].reshape(rows, wide)
        vdt = dot(vp, cs[h], 1, 1)
        vdo = dot(v_ref[:, c : c + wide], cs[h], 1, 1)
        weights, own = wt[h], wo[h]
        delta = jnp.sum(weights * vdt, axis=0, keepdims=True) + jnp.sum(own * vdo, axis=0, keepdims=True)
        dst = (weights * (vdt - delta)).astype(BF16)
        dso = (own * (vdo - delta)).astype(BF16)
        dq = (dot(dst, kp, 0, 0) + dot(dso, k_ref[:, c : c + wide], 0, 0)) * scale
        dq = jnp.where(low, dq[:tok], dq[tok:]).astype(BF16)
        gq_ref[:, c : c + wide] = dq
        dqr[j, :, c : c + wide] = dq
        dks[:, :, c : c + wide] = (dot(dst, qs[h], 1, 0) * scale).astype(BF16).reshape(n, BLK, wide)
        gko[:, c : c + wide] = dot(dso, qs[h], 1, 0) * scale

    def dq_copy(p, slot):
        return pltpu.make_async_remote_copy(
            src_ref=dqr.at[j], dst_ref=dqr.at[slot], send_sem=gssem.at[0, p], recv_sem=grsem.at[0, slot],
            device_id=(z * g + p, t), device_id_type=MESH)

    for i in range(1, g):
        dq_copy(lax.rem(j + i, g), j).start()
    each_lower(lambda o: tile_copy(3, dks.at[o], dkr.at[me], o, me).start())

    each_x(lambda p, t2: x_landed(p, t2).wait_recv())
    for i in range(1, g):
        p = lax.rem(j + i, g)
        dq_copy(p, p).wait_recv()

    def partial(zz):
        return dot(xr[:, zz].reshape(g * tok, w), dqr[...].reshape(g * tok, cols), 0, 0)

    def gw_copy(zz, slot):
        return pltpu.make_async_remote_copy(
            src_ref=gs.at[zz], dst_ref=gr.at[slot], send_sem=gssem.at[1, zz], recv_sem=grsem.at[1, slot],
            device_id=(zz * g + j, t), device_id_type=MESH)

    for i in range(1, r):
        zz = lax.rem(z + i, r)
        gs[zz] = partial(zz).astype(BF16)
        gw_copy(zz, z).start()
    gw_ref[...] = partial(z)

    def settle(kind, held, landed, own, out):
        def add(d):
            tile_copy(kind, held.at[d], landed.at[d], d, d).wait_recv()
            tile = landed[d].astype(F32)
            for b in range(bd):
                own[b * BLK : (b + 1) * BLK, :] += tile * hot_ref[d, b : b + 1, :]
        each_upper(add)
        out[...] = own[...].astype(BF16)

    settle(2, dvs, dvr, gvo, gv_ref)
    settle(3, dks, dkr, gko, gk_ref)
    for i in range(1, r):
        zz = lax.rem(z + i, r)
        gw_copy(zz, zz).wait_recv()
        gw_ref[...] += gr[zz].astype(F32)

    each_upper(lambda d: tile_copy(0, ks.at[d], kt.at[me], d, me).wait_send())
    each_upper(lambda d: tile_copy(1, vs.at[d], vt.at[me], d, me).wait_send())
    each_lower(lambda o: tile_copy(2, dvs.at[o], dvr.at[me], o, me).wait_send())
    each_lower(lambda o: tile_copy(3, dks.at[o], dkr.at[me], o, me).wait_send())
    each_x(lambda p, t2: x_copy(p, t2).wait_send())
    for i in range(1, g):
        dq_copy(lax.rem(j + i, g), j).wait_send()
    for i in range(1, r):
        gw_copy(lax.rem(z + i, r), z).wait_send()


def body(n, tp, g, queries, keys, values, cotangent, log_sum, chosen, normed_input):
    tok, cols = queries.shape
    heads = log_sum.shape[0]
    bd = tok // BLK
    pairs = heads // 2
    r = n // g
    sel = chosen.shape[2]
    me = lax.axis_index("kv")
    blocks = chosen.shape[1]
    ids = jnp.arange(blocks, dtype=jnp.int32)
    devs = jnp.arange(n, dtype=jnp.int32)
    own_ids = me * bd + jnp.arange(bd, dtype=jnp.int32)
    mine = lax.dynamic_slice_in_dim(chosen, me * bd, bd, 1)
    usable = mine < own_ids[None, :, None]
    owner = jnp.where(usable, mine // bd, n)
    tile_need = jnp.any(owner[:, None] == devs[None, :, None, None], axis=3) & (devs < me)[None, :, None]
    own_need = jnp.any((mine[:, None] == own_ids[None, :, None, None]) & usable[:, None], axis=3)
    need = jnp.concatenate([tile_need, own_need, jnp.ones((heads, 1, bd), bool)], axis=1)
    less = -log_sum.reshape(heads, 1, bd, BLK)
    bias = jnp.where(need[..., None], less, MASKED).reshape(pairs, 2, n + bd + 1, tok)
    bias = bias.transpose(0, 2, 1, 3).reshape(pairs, n + bd + 1, 1, 2 * tok)
    grouped = chosen.reshape(heads, n, 1, bd * sel)
    hot = jnp.any(grouped == own_ids[None, None, :, None], axis=3) & (devs > me)[None, :, None]
    hot = jnp.repeat(hot.transpose(1, 2, 0).astype(F32), HD, axis=2)
    w = normed_input.shape[1] // (r // tp * g)
    tile = (n, BLK, cols)
    vmem = pl.BlockSpec(memory_space=pltpu.VMEM)
    return pl.pallas_call(
        functools.partial(kernel, n, tp, g),
        out_shape=[
            jax.ShapeDtypeStruct((tok, cols), BF16),
            jax.ShapeDtypeStruct((tok, cols), BF16),
            jax.ShapeDtypeStruct((tok, cols), BF16),
            jax.ShapeDtypeStruct((w, cols), F32),
        ],
        in_specs=[vmem] * 7,
        out_specs=[vmem] * 4,
        scratch_shapes=[pltpu.VMEM(tile, BF16)] * 8
        + [
            pltpu.VMEM((pairs, n * BLK, 2 * tok), F32),
            pltpu.VMEM((pairs, tok, 2 * tok), F32),
            pltpu.VMEM((tok, cols), F32),
            pltpu.VMEM((tok, cols), F32),
            pltpu.VMEM((pairs, 2 * tok, 2 * HD), BF16),
            pltpu.VMEM((pairs, 2 * tok, 2 * HD), BF16),
            pltpu.VMEM((g, r // tp, tok, w), BF16),
            pltpu.VMEM((g, r, tok, w), BF16),
            pltpu.VMEM((g, tok, cols), BF16),
            pltpu.VMEM((r, w, cols), BF16),
            pltpu.VMEM((r, w, cols), BF16),
            pltpu.SemaphoreType.DMA((4, n)),
            pltpu.SemaphoreType.DMA((4, n)),
            pltpu.SemaphoreType.DMA((g, tp)),
            pltpu.SemaphoreType.DMA((g, tp)),
            pltpu.SemaphoreType.DMA((2, max(g, r))),
            pltpu.SemaphoreType.DMA((2, max(g, r))),
        ],
        compiler_params=pltpu.CompilerParams(has_side_effects=True, vmem_limit_bytes=48 * 1024 * 1024),
    )(queries, keys, values, cotangent, bias, hot, normed_input)


def solution(mesh):
    n, tp = mesh.shape["kv"], mesh.shape["tp"]
    g = 1
    while 4 * g * g <= n:
        g *= 2
    in_specs = (
        P("kv", "tp"), P("kv", "tp"), P("kv", "tp"), P("kv", "tp"),
        P("tp", "kv"), P("tp", None, None), P("kv", "tp"),
    )
    out_specs = (P("kv", "tp"),) * 4
    return jax.shard_map(
        functools.partial(body, n, tp, g), mesh=mesh, in_specs=in_specs, out_specs=out_specs, check_vma=False
    )
```

```python
import functools

import jax
import jax.numpy as jnp
from jax import lax
from jax.experimental import pallas as pl
from jax.experimental.pallas import tpu as pltpu
from jax.sharding import PartitionSpec as P

HD = 64
BLK = 32
MASKED = -1e30
MESH = pl.DeviceIdType.MESH
F32 = jnp.float32
BF16 = jnp.bfloat16


def dot(a, b, ca, cb):
    return lax.dot_general(a, b, (((ca,), (cb,)), ((), ())), preferred_element_type=F32)


def kernel(
    n, tp, g, q_ref, k_ref, v_ref, c_ref, lse_ref, pick_ref, x_ref,
    gq_ref, gk_ref, gv_ref, gw_ref,
    bias, hot, kvs, kvt, dkvs, dkvr, gko, gvo, xs, xr, dqr, gs, gr,
    ssem, rsem, xssem, xrsem, dssem, drsem, gssem, grsem,
):
    r = n // g
    tok, cols = q_ref.shape
    sel, heads, blocks = pick_ref.shape
    bd = tok // BLK
    wide = 2 * HD
    pairs = cols // wide
    scale = HD ** (-0.5)
    rt = r // tp
    w = x_ref.shape[1] // (rt * g)
    me, t = lax.axis_index("kv"), lax.axis_index("tp")
    z, j = me // g, lax.rem(me, g)
    rows = n * BLK

    def iota(shape, dim):
        return lax.broadcasted_iota(jnp.int32, shape, dim)

    def each(low, high, fn):
        def step(i, carry):
            fn(i)
            return carry
        lax.fori_loop(low, high, step, 0)

    def kv_copy(h, there, slot):
        return pltpu.make_async_remote_copy(
            src_ref=kvs.at[h, there], dst_ref=kvt.at[h, slot], send_sem=ssem.at[0, h, there],
            recv_sem=rsem.at[0, h, slot], device_id=(there, t), device_id_type=MESH)

    def back_copy(h, there, slot):
        return pltpu.make_async_remote_copy(
            src_ref=dkvs.at[h, there], dst_ref=dkvr.at[h, slot], send_sem=ssem.at[1, h, there],
            recv_sem=rsem.at[1, h, slot], device_id=(there, t), device_id_type=MESH)

    def x_copy(p, t2, at, t3):
        return pltpu.make_async_remote_copy(
            src_ref=xs.at[p], dst_ref=xr.at[at, pl.ds(t3 * rt, rt)],
            send_sem=xssem.at[p, t2], recv_sem=xrsem.at[at, t3],
            device_id=(z * g + p, t2), device_id_type=MESH)

    def dq_copy(h, p, slot):
        return pltpu.make_async_remote_copy(
            src_ref=dqr.at[h, j], dst_ref=dqr.at[h, slot], send_sem=dssem.at[h, p], recv_sem=drsem.at[h, slot],
            device_id=(z * g + p, t), device_id_type=MESH)

    def gw_copy(h, zz, slot):
        return pltpu.make_async_remote_copy(
            src_ref=gs.at[h, zz], dst_ref=gr.at[h, slot], send_sem=gssem.at[h, zz], recv_sem=grsem.at[h, slot],
            device_id=(zz * g + j, t), device_id_type=MESH)

    def each_x(fn):
        def step(i):
            p, t2 = i // tp, lax.rem(i, tp)

            @pl.when((p != j) | (t2 != t))
            def _():
                fn(p, t2)
        each(0, g * tp, step)

    pool = (iota((blocks, n), 0) // bd == iota((blocks, n), 1)).astype(BF16)
    spread = (iota((heads, cols), 1) // HD == iota((heads, cols), 0)).astype(BF16)
    later = iota((n, cols), 0) > me
    for b in range(bd):
        hit = jnp.zeros((heads, blocks), jnp.bool_)
        for s in range(sel):
            hit = hit | (pick_ref[s] == me * bd + b)
        count = dot(jnp.where(hit, 1.0, 0.0).astype(BF16), pool, 1, 0)
        taken = dot(count.astype(BF16), spread, 0, 0)
        hot[:, b, :] = jnp.where((taken > 0.5) & later, 1.0, 0.0)

    def picked(ref, d, c):
        out = None
        for b in range(bd):
            one = jnp.broadcast_to(hot[d, b : b + 1, c : c + wide], (BLK, wide)).astype(BF16)
            term = ref[b * BLK : (b + 1) * BLK, c : c + wide] * one
            out = term if out is None else out + term
        return out

    def send_kv(h):
        def step(i):
            d = n - 1 - i
            kvs[h, d, 0] = picked(k_ref, d, h * wide)
            kvs[h, d, 1] = picked(v_ref, d, h * wide)
            kv_copy(h, d, me).start()
        each(0, n - 1 - me, step)

    for h in range(pairs):
        send_kv(h)

    for p in range(g):
        for zl in range(rt):
            at = (zl * g + p) * w
            xs[p, zl] = x_ref[:, at : at + w]
    each_x(lambda p, t2: x_copy(p, t2, j, t).start())
    xr[j, pl.ds(t * rt, rt)] = xs[j]

    def clear(o):
        for h in range(pairs):
            kvt[h, o] = jnp.zeros(kvt.shape[2:], BF16)
    each(me, n, clear)

    at_block = me * bd + iota((blocks, tok), 1) // BLK
    mine = (iota((blocks, tok), 0) == at_block).astype(F32)
    ids = pick_ref[...].astype(F32).reshape(sel * heads, blocks)
    ids = dot(ids.astype(BF16), mine.astype(BF16), 1, 0)
    ids = (ids + 0.5).astype(jnp.int32).reshape(sel, heads, tok)
    ids = jnp.where(ids < me * bd + iota(ids.shape, 2) // BLK, ids, n * bd)
    owner = ids // bd
    less = -lse_ref[...]

    def put(row, need):
        line = less if need is None else jnp.where(need, less, MASKED)
        for h in range(heads):
            bias[h // 2, row, :, (h % 2) * tok : (h % 2 + 1) * tok] = line[h : h + 1, :]

    for o in range(n):
        need = jnp.zeros((heads, tok), jnp.bool_)
        for s in range(sel):
            need = need | (owner[s] == o)
        put(o, need & (jnp.zeros((heads, tok), jnp.int32) + o < me))
    for b in range(bd):
        need = jnp.zeros((heads, tok), jnp.bool_)
        for s in range(sel):
            need = need | (ids[s] == me * bd + b)
        put(n + b, need)
    put(n + bd, None)

    low = iota((tok, wide), 1) < HD
    key_at = iota((tok, 2 * tok), 0)
    query_at = lax.rem(iota((tok, 2 * tok), 1), tok)
    causal = (key_at // BLK == query_at // BLK) & (key_at <= query_at)

    def stacked(ref, c):
        part = ref[:, c : c + wide]
        zero = jnp.zeros_like(part)
        return jnp.concatenate([jnp.where(low, part, zero), jnp.where(low, zero, part)], axis=0)

    def attend(h):
        c = h * wide
        qs, cs = stacked(q_ref, c), stacked(c_ref, c)
        ko, vo = k_ref[:, c : c + wide], v_ref[:, c : c + wide]
        ob = jnp.broadcast_to(bias[h, n : n + bd], (bd, BLK, 2 * tok)).reshape(tok, 2 * tok)
        ob = jnp.where(causal, bias[h, n + bd], ob)
        own = jnp.exp(dot(ko, qs, 1, 1) * scale + ob)
        vdo = dot(vo, cs, 1, 1)
        gvo[:, c : c + wide] = dot(own.astype(BF16), cs, 1, 0)
        each(0, me, lambda o: kv_copy(h, o, o).wait_recv())
        kp = kvt[h, :, 0].reshape(rows, wide)
        vp = kvt[h, :, 1].reshape(rows, wide)
        st = (dot(kp, qs, 1, 1) * scale).reshape(n, BLK, 2 * tok)
        weights = jnp.exp(st + bias[h, :n]).reshape(rows, 2 * tok)
        vdt = dot(vp, cs, 1, 1)
        dkvs[h, :, 1] = dot(weights.astype(BF16), cs, 1, 0).astype(BF16).reshape(n, BLK, wide)
        delta = jnp.sum(weights * vdt, axis=0, keepdims=True) + jnp.sum(own * vdo, axis=0, keepdims=True)
        dst = (weights * (vdt - delta)).astype(BF16)
        dso = (own * (vdo - delta)).astype(BF16)
        dq = (dot(dst, kp, 0, 0) + dot(dso, ko, 0, 0)) * scale
        dq = jnp.where(low, dq[:tok], dq[tok:]).astype(BF16)
        gq_ref[:, c : c + wide] = dq
        dqr[h, j] = dq
        dkvs[h, :, 0] = (dot(dst, qs, 1, 0) * scale).astype(BF16).reshape(n, BLK, wide)
        for i in range(1, g):
            dq_copy(h, lax.rem(j + i, g), j).start()
        each(0, me, lambda o: back_copy(h, o, me).start())
        gko[:, c : c + wide] = dot(dso, qs, 1, 0) * scale

    def weight(h):
        for i in range(1, g):
            p = lax.rem(j + i, g)
            dq_copy(h, p, p).wait_recv()
        right = dqr[h].reshape(g * tok, wide)
        for i in range(1, r):
            zz = lax.rem(z + i, r)
            gs[h, zz] = dot(xr[:, zz].reshape(g * tok, w), right, 0, 0).astype(BF16)
            gw_copy(h, zz, z).start()
        gw_ref[:, h * wide : (h + 1) * wide] = dot(xr[:, z].reshape(g * tok, w), right, 0, 0)

    for h in range(pairs):
        attend(h)
        if h == 0:
            each_x(lambda p, t2: x_copy(p, t2, p, t2).wait_recv())
        else:
            weight(h - 1)
    weight(pairs - 1)

    for h in range(pairs):
        c = h * wide

        def add(d):
            back_copy(h, d, d).wait_recv()
            dk, dv = dkvr[h, d, 0].astype(F32), dkvr[h, d, 1].astype(F32)
            for b in range(bd):
                one = hot[d, b : b + 1, c : c + wide]
                gko[b * BLK : (b + 1) * BLK, c : c + wide] += dk * one
                gvo[b * BLK : (b + 1) * BLK, c : c + wide] += dv * one
        each(me + 1, n, add)
        gk_ref[:, c : c + wide] = gko[:, c : c + wide].astype(BF16)
        gv_ref[:, c : c + wide] = gvo[:, c : c + wide].astype(BF16)
        for i in range(1, r):
            zz = lax.rem(z + i, r)
            gw_copy(h, zz, zz).wait_recv()
            gw_ref[:, c : c + wide] += gr[h, zz].astype(F32)

    for h in range(pairs):
        each(me + 1, n, lambda d: kv_copy(h, d, me).wait_send())
        each(0, me, lambda o: back_copy(h, o, me).wait_send())
        for i in range(1, g):
            dq_copy(h, lax.rem(j + i, g), j).wait_send()
        for i in range(1, r):
            gw_copy(h, lax.rem(z + i, r), z).wait_send()
    each_x(lambda p, t2: x_copy(p, t2, j, t).wait_send())


def body(n, tp, g, queries, keys, values, cotangent, log_sum, chosen, normed_input):
    tok, cols = queries.shape
    wide = 2 * HD
    pairs = cols // wide
    bd = tok // BLK
    r = n // g
    w = normed_input.shape[1] // (r // tp * g)
    tiles = pltpu.VMEM((pairs, n, 2, BLK, wide), BF16)
    vmem = pl.BlockSpec(memory_space=pltpu.VMEM)
    sem = pltpu.SemaphoreType.DMA
    return pl.pallas_call(
        functools.partial(kernel, n, tp, g),
        out_shape=[
            jax.ShapeDtypeStruct((tok, cols), BF16),
            jax.ShapeDtypeStruct((tok, cols), BF16),
            jax.ShapeDtypeStruct((tok, cols), BF16),
            jax.ShapeDtypeStruct((w, cols), F32),
        ],
        in_specs=[vmem] * 7,
        out_specs=[vmem] * 4,
        scratch_shapes=[
            pltpu.VMEM((pairs, n + bd + 1, 1, 2 * tok), F32),
            pltpu.VMEM((n, bd, cols), F32),
            tiles, tiles, tiles, tiles,
            pltpu.VMEM((tok, cols), F32),
            pltpu.VMEM((tok, cols), F32),
            pltpu.VMEM((g, r // tp, tok, w), BF16),
            pltpu.VMEM((g, r, tok, w), BF16),
            pltpu.VMEM((pairs, g, tok, wide), BF16),
            pltpu.VMEM((pairs, r, w, wide), BF16),
            pltpu.VMEM((pairs, r, w, wide), BF16),
            sem((2, pairs, n)), sem((2, pairs, n)),
            sem((g, tp)), sem((g, tp)),
            sem((pairs, g)), sem((pairs, g)),
            sem((pairs, r)), sem((pairs, r)),
        ],
        compiler_params=pltpu.CompilerParams(has_side_effects=True, vmem_limit_bytes=48 * 1024 * 1024),
    )(queries, keys, values, cotangent, log_sum, chosen.transpose(2, 0, 1), normed_input)


def solution(mesh):
    n, tp = mesh.shape["kv"], mesh.shape["tp"]
    g = 1
    while 4 * g * g <= n:
        g *= 2
    in_specs = (
        P("kv", "tp"), P("kv", "tp"), P("kv", "tp"), P("kv", "tp"),
        P("tp", "kv"), P("tp", None, None), P("kv", "tp"),
    )
    out_specs = (P("kv", "tp"),) * 4
    return jax.shard_map(
        functools.partial(body, n, tp, g), mesh=mesh, in_specs=in_specs, out_specs=out_specs, check_vma=False
    )
```

```python
import functools

import jax
import jax.numpy as jnp
from jax import lax
from jax.experimental import pallas as pl
from jax.experimental.pallas import tpu as pltpu
from jax.sharding import PartitionSpec as P

HD = 64
BLK = 32
MASKED = -1e30
MESH = pl.DeviceIdType.MESH
F32 = jnp.float32
BF16 = jnp.bfloat16


def dot(a, b, ca, cb):
    return lax.dot_general(a, b, (((ca,), (cb,)), ((), ())), preferred_element_type=F32)


def kernel(
    n, tp, g, q_in, k_in, v_in, c_in, lse_in, pick_in, x_in,
    gq_ref, gk_ref, gv_ref, gw_ref,
    q_ref, k_ref, v_ref, c_ref, lse_ref, pick_ref, x_ref, insem, bias, hot, kvs, kvt, dkvs, dkvr, gko, gvo, xs, xr, dqr, gs, gr,
    ssem, rsem, xssem, xrsem, dssem, drsem, gssem, grsem,
):
    r = n // g
    tok, cols = q_ref.shape
    sel, heads, blocks = pick_ref.shape
    bd = tok // BLK
    wide = 2 * HD
    pairs = cols // wide
    scale = HD ** (-0.5)
    rt = r // tp
    w = x_ref.shape[1] // (rt * g)
    me, t = lax.axis_index("kv"), lax.axis_index("tp")
    z, j = me // g, lax.rem(me, g)
    rows = n * BLK

    loads = {}
    for i, (a, b) in enumerate((
        (pick_in, pick_ref), (k_in, k_ref), (v_in, v_ref), (x_in, x_ref),
        (q_in, q_ref), (c_in, c_ref), (lse_in, lse_ref),
    )):
        loads[i] = pltpu.make_async_copy(a, b, insem.at[i])
        loads[i].start()

    def iota(shape, dim):
        return lax.broadcasted_iota(jnp.int32, shape, dim)

    def each(low, high, fn):
        def step(i, carry):
            fn(i)
            return carry
        lax.fori_loop(low, high, step, 0)

    def kv_copy(h, there, slot):
        return pltpu.make_async_remote_copy(
            src_ref=kvs.at[h, there], dst_ref=kvt.at[h, slot], send_sem=ssem.at[0, h, there],
            recv_sem=rsem.at[0, h, slot], device_id=(there, t), device_id_type=MESH)

    def back_copy(h, there, slot):
        return pltpu.make_async_remote_copy(
            src_ref=dkvs.at[h, there], dst_ref=dkvr.at[h, slot], send_sem=ssem.at[1, h, there],
            recv_sem=rsem.at[1, h, slot], device_id=(there, t), device_id_type=MESH)

    def x_copy(p, t2, at, t3):
        return pltpu.make_async_remote_copy(
            src_ref=xs.at[p], dst_ref=xr.at[at, pl.ds(t3 * rt, rt)],
            send_sem=xssem.at[p, t2], recv_sem=xrsem.at[at, t3],
            device_id=(z * g + p, t2), device_id_type=MESH)

    def dq_copy(h, p, slot):
        return pltpu.make_async_remote_copy(
            src_ref=dqr.at[h, j], dst_ref=dqr.at[h, slot], send_sem=dssem.at[h, p], recv_sem=drsem.at[h, slot],
            device_id=(z * g + p, t), device_id_type=MESH)

    def gw_copy(h, zz, slot):
        return pltpu.make_async_remote_copy(
            src_ref=gs.at[h, zz], dst_ref=gr.at[h, slot], send_sem=gssem.at[h, zz], recv_sem=grsem.at[h, slot],
            device_id=(zz * g + j, t), device_id_type=MESH)

    def each_x(fn):
        def step(i):
            p, t2 = lax.rem(j + i // tp, g), lax.rem(i, tp)

            @pl.when((p != j) | (t2 != t))
            def _():
                fn(p, t2)
        each(0, g * tp, step)

    pool = (iota((blocks, n), 0) // bd == iota((blocks, n), 1)).astype(BF16)
    spread = (iota((heads, cols), 1) // HD == iota((heads, cols), 0)).astype(BF16)
    later = iota((n, cols), 0) > me
    loads[0].wait()
    for b in range(bd):
        hit = jnp.zeros((heads, blocks), jnp.bool_)
        for s in range(sel):
            hit = hit | (pick_ref[s] == me * bd + b)
        count = dot(jnp.where(hit, 1.0, 0.0).astype(BF16), pool, 1, 0)
        taken = dot(count.astype(BF16), spread, 0, 0)
        hot[:, b, :] = jnp.where((taken > 0.5) & later, 1.0, 0.0)

    def picked(ref, d, c):
        out = None
        for b in range(bd):
            one = jnp.broadcast_to(hot[d, b : b + 1, c : c + wide], (BLK, wide)).astype(BF16)
            term = ref[b * BLK : (b + 1) * BLK, c : c + wide] * one
            out = term if out is None else out + term
        return out

    def send_kv(h):
        def step(i):
            d = (r - 1 - i // g) * g + lax.rem(j + lax.rem(i, g), g)

            @pl.when(d > me)
            def _():
                kvs[h, d, 0] = picked(k_ref, d, h * wide)
                kvs[h, d, 1] = picked(v_ref, d, h * wide)
                kv_copy(h, d, me).start()
        each(0, (r - z) * g, step)

    def send_back(h):
        def step(i):
            o = (i // g) * g + lax.rem(j + lax.rem(i, g), g)

            @pl.when(o < me)
            def _():
                back_copy(h, o, me).start()
        each(0, (z + 1) * g, step)

    loads[1].wait()
    loads[2].wait()
    for h in range(pairs):
        send_kv(h)

    loads[3].wait()
    for p in range(g):
        for zl in range(rt):
            at = (zl * g + p) * w
            xs[p, zl] = x_ref[:, at : at + w]
    each_x(lambda p, t2: x_copy(p, t2, j, t).start())
    xr[j, pl.ds(t * rt, rt)] = xs[j]

    def clear(o):
        for h in range(pairs):
            kvt[h, o] = jnp.zeros(kvt.shape[2:], BF16)
    each(me, n, clear)

    at_block = me * bd + iota((blocks, tok), 1) // BLK
    mine = (iota((blocks, tok), 0) == at_block).astype(F32)
    ids = pick_ref[...].astype(F32).reshape(sel * heads, blocks)
    ids = dot(ids.astype(BF16), mine.astype(BF16), 1, 0)
    ids = (ids + 0.5).astype(jnp.int32).reshape(sel, heads, tok)
    ids = jnp.where(ids < me * bd + iota(ids.shape, 2) // BLK, ids, n * bd)
    owner = ids // bd
    for i in (4, 5, 6):
        loads[i].wait()
    less = -lse_ref[...]

    def put(row, need):
        line = less if need is None else jnp.where(need, less, MASKED)
        for h in range(heads):
            bias[h // 2, row, :, (h % 2) * tok : (h % 2 + 1) * tok] = line[h : h + 1, :]

    for o in range(n):
        need = jnp.zeros((heads, tok), jnp.bool_)
        for s in range(sel):
            need = need | (owner[s] == o)
        put(o, need & (jnp.zeros((heads, tok), jnp.int32) + o < me))
    for b in range(bd):
        need = jnp.zeros((heads, tok), jnp.bool_)
        for s in range(sel):
            need = need | (ids[s] == me * bd + b)
        put(n + b, need)
    put(n + bd, None)

    low = iota((tok, wide), 1) < HD
    key_at = iota((tok, 2 * tok), 0)
    query_at = lax.rem(iota((tok, 2 * tok), 1), tok)
    causal = (key_at // BLK == query_at // BLK) & (key_at <= query_at)

    def stacked(ref, c):
        part = ref[:, c : c + wide]
        zero = jnp.zeros_like(part)
        return jnp.concatenate([jnp.where(low, part, zero), jnp.where(low, zero, part)], axis=0)

    def attend(h):
        c = h * wide
        qs, cs = stacked(q_ref, c), stacked(c_ref, c)
        ko, vo = k_ref[:, c : c + wide], v_ref[:, c : c + wide]
        ob = jnp.broadcast_to(bias[h, n : n + bd], (bd, BLK, 2 * tok)).reshape(tok, 2 * tok)
        ob = jnp.where(causal, bias[h, n + bd], ob)
        own = jnp.exp(dot(ko, qs, 1, 1) * scale + ob)
        vdo = dot(vo, cs, 1, 1)
        gvo[:, c : c + wide] = dot(own.astype(BF16), cs, 1, 0)
        each(0, me, lambda o: kv_copy(h, o, o).wait_recv())
        kp = kvt[h, :, 0].reshape(rows, wide)
        vp = kvt[h, :, 1].reshape(rows, wide)
        st = (dot(kp, qs, 1, 1) * scale).reshape(n, BLK, 2 * tok)
        weights = jnp.exp(st + bias[h, :n]).reshape(rows, 2 * tok)
        vdt = dot(vp, cs, 1, 1)
        dkvs[h, :, 1] = dot(weights.astype(BF16), cs, 1, 0).astype(BF16).reshape(n, BLK, wide)
        delta = jnp.sum(weights * vdt, axis=0, keepdims=True) + jnp.sum(own * vdo, axis=0, keepdims=True)
        dst = (weights * (vdt - delta)).astype(BF16)
        dso = (own * (vdo - delta)).astype(BF16)
        dq = (dot(dst, kp, 0, 0) + dot(dso, ko, 0, 0)) * scale
        dq = jnp.where(low, dq[:tok], dq[tok:]).astype(BF16)
        gq_ref[:, c : c + wide] = dq
        dqr[h, j] = dq
        dkvs[h, :, 0] = (dot(dst, qs, 1, 0) * scale).astype(BF16).reshape(n, BLK, wide)
        for i in range(1, g):
            dq_copy(h, lax.rem(j + i, g), j).start()
        send_back(h)
        gko[:, c : c + wide] = dot(dso, qs, 1, 0) * scale

    def weight(h):
        for i in range(1, g):
            p = lax.rem(j + i, g)
            dq_copy(h, p, p).wait_recv()
        right = dqr[h].reshape(g * tok, wide)
        for i in range(1, r):
            zz = lax.rem(z + i, r)
            gs[h, zz] = dot(xr[:, zz].reshape(g * tok, w), right, 0, 0).astype(BF16)
            gw_copy(h, zz, z).start()
        gw_ref[:, h * wide : (h + 1) * wide] = dot(xr[:, z].reshape(g * tok, w), right, 0, 0)

    for h in range(pairs):
        attend(h)
        if h == 0:
            each_x(lambda p, t2: x_copy(p, t2, p, t2).wait_recv())
        else:
            weight(h - 1)
    weight(pairs - 1)

    for h in range(pairs):
        c = h * wide

        def add(d):
            back_copy(h, d, d).wait_recv()
            dk, dv = dkvr[h, d, 0].astype(F32), dkvr[h, d, 1].astype(F32)
            for b in range(bd):
                one = hot[d, b : b + 1, c : c + wide]
                gko[b * BLK : (b + 1) * BLK, c : c + wide] += dk * one
                gvo[b * BLK : (b + 1) * BLK, c : c + wide] += dv * one
        each(me + 1, n, add)
        gk_ref[:, c : c + wide] = gko[:, c : c + wide].astype(BF16)
        gv_ref[:, c : c + wide] = gvo[:, c : c + wide].astype(BF16)
        for i in range(1, r):
            zz = lax.rem(z + i, r)
            gw_copy(h, zz, zz).wait_recv()
            gw_ref[:, c : c + wide] += gr[h, zz].astype(F32)

    for h in range(pairs):
        each(me + 1, n, lambda d: kv_copy(h, d, me).wait_send())
        each(0, me, lambda o: back_copy(h, o, me).wait_send())
        for i in range(1, g):
            dq_copy(h, lax.rem(j + i, g), j).wait_send()
        for i in range(1, r):
            gw_copy(h, lax.rem(z + i, r), z).wait_send()
    each_x(lambda p, t2: x_copy(p, t2, j, t).wait_send())


def write_out(*refs):
    sems = refs[8]
    copies = [pltpu.make_async_copy(refs[i], refs[4 + i], sems.at[i]) for i in range(4)]
    for copy in copies:
        copy.start()
    for copy in copies:
        copy.wait()


def body(n, tp, g, queries, keys, values, cotangent, log_sum, chosen, normed_input):
    tok, cols = queries.shape
    wide = 2 * HD
    pairs = cols // wide
    bd = tok // BLK
    r = n // g
    w = normed_input.shape[1] // (r // tp * g)
    tiles = pltpu.VMEM((pairs, n, 2, BLK, wide), BF16)
    vmem = pl.BlockSpec(memory_space=pltpu.VMEM)
    sem = pltpu.SemaphoreType.DMA
    hbm = pl.BlockSpec(memory_space=pltpu.HBM)
    picks = chosen.transpose(2, 0, 1)
    held = [pltpu.VMEM(a.shape, a.dtype) for a in (
        queries, keys, values, cotangent, log_sum, picks, normed_input)]
    made = pl.pallas_call(
        functools.partial(kernel, n, tp, g),
        out_shape=[
            jax.ShapeDtypeStruct((tok, cols), BF16),
            jax.ShapeDtypeStruct((tok, cols), BF16),
            jax.ShapeDtypeStruct((tok, cols), BF16),
            jax.ShapeDtypeStruct((w, cols), F32),
        ],
        in_specs=[hbm] * 7,
        out_specs=[vmem] * 4,
        scratch_shapes=held + [
            sem((7,)),
            pltpu.VMEM((pairs, n + bd + 1, 1, 2 * tok), F32),
            pltpu.VMEM((n, bd, cols), F32),
            tiles, tiles, tiles, tiles,
            pltpu.VMEM((tok, cols), F32),
            pltpu.VMEM((tok, cols), F32),
            pltpu.VMEM((g, r // tp, tok, w), BF16),
            pltpu.VMEM((g, r, tok, w), BF16),
            pltpu.VMEM((pairs, g, tok, wide), BF16),
            pltpu.VMEM((pairs, r, w, wide), BF16),
            pltpu.VMEM((pairs, r, w, wide), BF16),
            sem((2, pairs, n)), sem((2, pairs, n)),
            sem((g, tp)), sem((g, tp)),
            sem((pairs, g)), sem((pairs, g)),
            sem((pairs, r)), sem((pairs, r)),
        ],
        compiler_params=pltpu.CompilerParams(has_side_effects=True, vmem_limit_bytes=67043328),
    )(queries, keys, values, cotangent, log_sum, picks, normed_input)
    return pl.pallas_call(
        write_out,
        out_shape=[jax.ShapeDtypeStruct(a.shape, a.dtype) for a in made],
        in_specs=[vmem] * 4,
        out_specs=[hbm] * 4,
        scratch_shapes=[sem((4,))],
    )(*made)


def solution(mesh):
    n, tp = mesh.shape["kv"], mesh.shape["tp"]
    g = 1
    while 4 * g * g <= n:
        g *= 2
    in_specs = (
        P("kv", "tp"), P("kv", "tp"), P("kv", "tp"), P("kv", "tp"),
        P("tp", "kv"), P("tp", None, None), P("kv", "tp"),
    )
    out_specs = (P("kv", "tp"),) * 4
    return jax.shard_map(
        functools.partial(body, n, tp, g), mesh=mesh, in_specs=in_specs, out_specs=out_specs, check_vma=False
    )
```
